32 devices in a mesh: ep: 8 (over z, y), tp: 4 (over x, core).
Axes of the slice: x: 2, y: 2, z: 4, core: 2. Of those that a mesh axis runs over, the one named last changes fastest.
Arguments:
- hidden_in: bfloat16 [384, 2048], P('ep'), may hold values from -6 to 6
- carried_state: float32 [384, 4, 128, 256], P('ep', 'tp'), may hold values from -6 to 6
- input_gain: bfloat16 [2048], replicated, may hold values from 0.099609375 to 1.8984375
- query_weight: bfloat16 [2048, 512], P(None, 'tp'), may hold values from -0.125 to 0.125
- key_weight: bfloat16 [2048, 512], P(None, 'tp'), may hold values from -0.125 to 0.125
- value_weight: bfloat16 [2048, 1024], P(None, 'tp'), may hold values from -0.125 to 0.125
- outgate_weight: bfloat16 [2048, 1024], P(None, 'tp'), may hold values from -0.125 to 0.125
- decay_weight: bfloat16 [2048, 512], P(None, 'tp'), may hold values from -0.5 to 0.5
- decay_shift: float32 [384, 512], P('ep', 'tp'), may hold values from -0.7 to 0
- head_gain: bfloat16 [4, 256], P('tp'), may hold values from 0.099609375 to 1.8984375
- output_weight: bfloat16 [1024, 2048], P('tp'), may hold values from -0.1875 to 0.1875
- channel_gain: bfloat16 [2048], replicated, may hold values from 0.099609375 to 1.8984375
- branch_gate: bfloat16 [2048], replicated, may hold values from -0.125 to 0.125
- routes: int32 [384, 2], P('ep'), may hold values from 0 to 7, all different within a row; in each aligned block of 48 rows (0 to 47, 48 to 95, ...) at most 14 rows name the same one
- route_weights: float32 [384, 2], P('ep'), may hold values from 0.1 to 1
- expert_gate: bfloat16 [8, 2048, 3072], P('ep', None, 'tp'), may hold values from -0.125 to 0.125
- expert_up: bfloat16 [8, 2048, 3072], P('ep', None, 'tp'), may hold values from -0.125 to 0.125
- expert_down: bfloat16 [8, 3072, 2048], P('ep', 'tp'), may hold values from -0.109375 to 0.109375
- dense_gate: bfloat16 [2048, 4096], P('tp', 'ep'), may hold values from -0.125 to 0.125
- dense_up: bfloat16 [2048, 4096], P('tp', 'ep'), may hold values from -0.125 to 0.125
- dense_down: bfloat16 [4096, 2048], P('ep', 'tp'), may hold values from -0.09375 to 0.09375
Outputs:
- mixed: bfloat16 [384, 2048], P('ep', 'tp')
- new_state: float32 [384, 4, 128, 256], P('ep', 'tp')
The draws below stay inside these ranges and needn't reach their ends.
Inputs may be any that keep to these rules, and one draw needn't show every extreme that they name: `routes`: each row names 2 different experts. Among the rows of one index of ep no expert is named more than 14 times, and in every draw some expert is named exactly 14 times by the rows of some index.
All inputs are finite; a program needn't handle non-finite values.
Results may differ from the reference program's by a relative error of at most 0.02.
Values may be sent and summed in bfloat16 or wider, within the bound.
No kernel may reach another device: no remote copies, remote signals or barrier semaphores. Data moves between devices by JAX's collectives and lax.ppermute only.
A program may use at most 128 MiB of HBM per device.

```python
import math
import jax
import jax.numpy as jnp
import numpy as np
from jax import lax

D = 2048
HEADS = 4
DK = 128
DV = 256
FF = 3072
DFF = 4096
TOPK = 2
SEQ_DEV = 48
BATCH = 384
EXPERTS = 8
CAP = 14
N_EP = 8
N_TP = 4


def level_of(stream_key, dims, pieces, smallest, largest):
    gain = 1.0
    for axis_at, blocks in pieces:
        draws = jax.random.uniform(jax.random.fold_in(jax.random.fold_in(stream_key, 6), axis_at), (blocks,), jnp.float32, smallest / len(pieces), largest / len(pieces))
        gain = gain * jnp.repeat(jnp.exp(draws), dims[axis_at] // blocks).reshape((-1,) + (1,) * (len(dims) - 1 - axis_at))
    return gain


def shared_out(key, own, number, rows, amount, top, limit, skew):
    ranking = jax.random.permutation(key, amount)
    crowded, common = shares(amount, rows * top, limit, skew, True), shares(amount, rows * top, limit, skew, False)
    places = jnp.arange(amount)

    def named(tallies, offset_by):
        used = int((tallies > 0).sum())
        fixed = max(1, used // 4)
        passed = fixed + (places - fixed + offset_by * (used - fixed)) % max(1, amount - fixed)
        return jnp.zeros((amount,), jnp.int32).at[ranking[jnp.where(places < fixed, places, passed)]].set(jnp.asarray(tallies, jnp.int32))

    tallies = jnp.where(number % 4 == 0, named(crowded, number // 4), named(common, number - number // 4 - 1))
    mixed = jax.random.permutation(jax.random.fold_in(own, 3), amount)
    donor, taker = mixed[0:amount // 2 * 2:2], mixed[1:amount // 2 * 2:2]
    slack = jnp.minimum(tallies[donor] - 1, limit - tallies[taker]) // 2
    slack = jnp.where((donor == ranking[0]) | (taker == ranking[0]) | (tallies[taker] == 0), 0, jnp.maximum(slack, 0))
    passed = jax.random.randint(jax.random.fold_in(own, 4), (amount // 2,), 0, 1 << 20) % (slack + 1)
    tallies = tallies.at[donor].add(-passed).at[taker].add(passed)
    members = jnp.searchsorted(jnp.cumsum(tallies), jnp.arange(rows * top), side="right").astype(jnp.int32)
    table = members.reshape(top, rows).T
    table = table[jax.random.permutation(jax.random.fold_in(own, 1), rows)]
    offset_by = jax.random.randint(jax.random.fold_in(own, 2), (rows, 1), 0, top)
    return jnp.take_along_axis(table, (jnp.arange(top)[None, :] + offset_by) % top, axis=1)


def shares(count, total, reach, slope, full):
    loads = [(1 << 20) // math.isqrt(standing ** slope) + 1 for standing in range(1, count + 1)]
    largest = reach if full else min(reach, max(-(-total // count), total * loads[0] // sum(loads)))
    least = 1 if total - largest >= count - 1 else 0
    counts, spare = [largest] + [least] * (count - 1), total - largest - least * (count - 1)
    while spare > 0:
        movable = [i for i in range(1, count) if counts[i] < largest] or [i for i in range(1, count) if counts[i] < reach]
        pool, remaining = sum([loads[i] for i in movable]), spare
        for i in movable:
            extra = min(reach - counts[i], max(1, remaining * loads[i] // pool), spare)
            counts[i] = counts[i] + extra
            spare = spare - extra
    return np.array(counts)


def gaussian(rng, dims, deviation, most, shards=(), held_as=jnp.bfloat16):
    values = deviation * jax.random.normal(rng, dims, jnp.float32)
    if shards:
        values = values * level_of(rng, dims, shards, -0.22, 0.18)
    return jnp.clip(values, -most, most).astype(held_as)


def setup_inputs(seed: int = 0) -> dict:
    streams_of = jax.random.split(jax.random.key(seed), 22)
    hidden_in = gaussian(streams_of[0], (BATCH, D), 1.0, 6.0, ((0, 8),))
    carried_state = gaussian(streams_of[1], (BATCH, HEADS, DK, DV), 1.0, 6.0, ((0, 8), (1, 4)), jnp.float32)
    input_gain = jnp.clip(1.0 + 0.18 * jax.random.normal(streams_of[2], (D,), jnp.float32), 0.099609375, 1.8984375).astype(jnp.bfloat16)
    query_weight = gaussian(streams_of[3], (D, HEADS * DK), D ** -0.5, 0.125, ((1, 4),))
    key_weight = gaussian(streams_of[4], (D, HEADS * DK), D ** -0.5, 0.125, ((1, 4),))
    value_weight = gaussian(streams_of[5], (D, HEADS * DV), D ** -0.5, 0.125, ((1, 4),))
    outgate_weight = gaussian(streams_of[6], (D, HEADS * DV), D ** -0.5, 0.125, ((1, 4),))
    decay_weight = gaussian(streams_of[7], (D, HEADS * DK), (D // 16) ** -0.5, 0.5, ((1, 4),))
    decay_shift = jnp.clip(-0.7 + 0.7 * jax.random.uniform(streams_of[8], (BATCH, HEADS * DK), jnp.float32) ** level_of(streams_of[8], (BATCH, HEADS * DK), ((0, 8), (1, 4)), -0.2, 0.2), -0.7, 0.0)
    head_gain = jnp.clip(1.0 + 0.18 * jax.random.normal(streams_of[9], (HEADS, DV), jnp.float32), 0.099609375, 1.8984375).astype(jnp.bfloat16)
    output_weight = gaussian(streams_of[10], (HEADS * DV, D), (HEADS * DV) ** -0.5, 0.1875, ((0, 4),))
    channel_gain = jnp.clip(1.0 + 0.18 * jax.random.normal(streams_of[11], (D,), jnp.float32), 0.099609375, 1.8984375).astype(jnp.bfloat16)
    branch_gate = gaussian(streams_of[12], (D,), D ** -0.5, 0.125)
    routes_keys = jax.random.split(jax.random.fold_in(streams_of[13], 1), BATCH // SEQ_DEV)
    routes_turns = jax.random.permutation(jax.random.fold_in(streams_of[13], 3), BATCH // SEQ_DEV)
    routes = jax.vmap(lambda own, number: shared_out(jax.random.fold_in(streams_of[13], 2), own, number, SEQ_DEV, EXPERTS, TOPK, CAP, 2))(routes_keys, routes_turns).reshape((BATCH, TOPK))
    route_weights = jnp.clip(0.1 + 0.9 * jax.random.uniform(streams_of[14], (BATCH, TOPK), jnp.float32) ** level_of(streams_of[14], (BATCH, TOPK), ((0, 8),), -0.2, 0.2), 0.1, 1.0)
    expert_gate = gaussian(streams_of[15], (EXPERTS, D, FF), D ** -0.5, 0.125, ((0, 8), (2, 4)))
    expert_up = gaussian(streams_of[16], (EXPERTS, D, FF), D ** -0.5, 0.125, ((0, 8), (2, 4)))
    expert_down = gaussian(streams_of[17], (EXPERTS, FF, D), FF ** -0.5, 0.109375, ((0, 8), (1, 4)))
    dense_gate = gaussian(streams_of[18], (D, DFF), D ** -0.5, 0.125, ((0, 4), (1, 8)))
    dense_up = gaussian(streams_of[19], (D, DFF), D ** -0.5, 0.125, ((0, 4), (1, 8)))
    dense_down = gaussian(streams_of[20], (DFF, D), DFF ** -0.5, 0.09375, ((0, 8), (1, 4)))
    return dict(hidden_in=hidden_in, carried_state=carried_state, input_gain=input_gain, query_weight=query_weight, key_weight=key_weight, value_weight=value_weight, outgate_weight=outgate_weight, decay_weight=decay_weight, decay_shift=decay_shift, head_gain=head_gain, output_weight=output_weight, channel_gain=channel_gain, branch_gate=branch_gate, routes=routes, route_weights=route_weights, expert_gate=expert_gate, expert_up=expert_up, expert_down=expert_down, dense_gate=dense_gate, dense_up=dense_up, dense_down=dense_down)


EPSILON = 1e-06
TAU_DECAY = 16.0

def rms_factor(values):
    return lax.rsqrt(lax.optimization_barrier(jnp.mean(values * values, axis=-1, keepdims=True)) + EPSILON)

def rounded(values):
    return lax.optimization_barrier(values.astype(jnp.bfloat16)).astype(jnp.float32)

def matmul(left, right):
    return jnp.dot(left, right, preferred_element_type=jnp.float32)

def expert_apply(token_rows, gate_matrix, up_matrix, down_matrix):
    block_width = gate_matrix.shape[1] // N_TP
    total = jnp.zeros((token_rows.shape[0], down_matrix.shape[1]), jnp.float32)
    for block in range(N_TP):
        lower = block * block_width
        gate_part = matmul(token_rows, gate_matrix[:, lower:lower + block_width])
        up_part = matmul(token_rows, up_matrix[:, lower:lower + block_width])
        hidden = (jax.nn.silu(gate_part) * up_part).astype(jnp.bfloat16)
        total = total + rounded(matmul(hidden, down_matrix[lower:lower + block_width]))
    return total

def reference(hidden_in, carried_state, input_gain, query_weight, key_weight, value_weight, outgate_weight, decay_weight, decay_shift, head_gain, output_weight, channel_gain, branch_gate, routes, route_weights, expert_gate, expert_up, expert_down, dense_gate, dense_up, dense_down):
    batch_size, width = hidden_in.shape
    head_count, key_dim, value_dim = carried_state.shape[1:]
    inputs = hidden_in.astype(jnp.float32)
    normed = (inputs * rms_factor(inputs) * input_gain.astype(jnp.float32)).astype(jnp.bfloat16)
    query = matmul(normed, query_weight).astype(jnp.bfloat16)
    key_rows = matmul(normed, key_weight).astype(jnp.bfloat16)
    value_rows = matmul(normed, value_weight).astype(jnp.bfloat16)
    outgate = matmul(normed, outgate_weight).astype(jnp.bfloat16)
    decay = jnp.exp(jax.nn.log_sigmoid(matmul(normed, decay_weight)) / TAU_DECAY + decay_shift)
    decay = decay.reshape(batch_size, head_count, key_dim)
    query_scaled = query.astype(jnp.float32).reshape(batch_size, head_count, key_dim) * key_dim ** (-0.5)
    key_vals = key_rows.astype(jnp.float32).reshape(batch_size, head_count, key_dim)
    value_vals = value_rows.astype(jnp.float32).reshape(batch_size, head_count, value_dim)
    new_state = decay[..., None] * carried_state + key_vals[..., None] * value_vals[:, :, None, :]
    readout = jnp.einsum('bhk,bhkv->bhv', query_scaled, new_state, precision=lax.Precision.HIGHEST)
    gate_vals = jax.nn.silu(outgate.astype(jnp.float32).reshape(batch_size, head_count, value_dim))
    gated = (readout * rms_factor(readout) * head_gain.astype(jnp.float32) * gate_vals).astype(jnp.bfloat16)
    group = head_count // N_TP
    attended = jnp.zeros((batch_size, width), jnp.float32)
    for block in range(N_TP):
        head_rows = gated[:, block * group:(block + 1) * group].reshape(batch_size, group * value_dim)
        weight_rows = output_weight[block * group * value_dim:(block + 1) * group * value_dim]
        attended = attended + rounded(matmul(head_rows, weight_rows))
    middle = rounded(inputs + attended)
    scaled = middle * rms_factor(middle) * channel_gain.astype(jnp.float32)
    branch = jax.nn.sigmoid(lax.optimization_barrier(jnp.sum(scaled * branch_gate.astype(jnp.float32), axis=-1)))
    ffn_in = scaled.astype(jnp.bfloat16)
    dense_hidden = (jax.nn.silu(matmul(ffn_in, dense_gate)) * matmul(ffn_in, dense_up)).astype(jnp.bfloat16)
    dense = matmul(dense_hidden, dense_down)
    topk = routes.shape[1]
    flat_routes = routes.reshape(-1)
    flat_tokens = (jnp.arange(flat_routes.shape[0], dtype=jnp.int32) // topk).astype(jnp.int32)
    flat_weights = route_weights.reshape(-1)
    capacity = N_EP * CAP

    def one_expert(carry, index):
        order = jnp.argsort((flat_routes != index).astype(jnp.int32), stable=True)[:capacity]
        valid = flat_routes[order] == index
        token_ids = flat_tokens[order]
        result = expert_apply(ffn_in[token_ids], expert_gate[index], expert_up[index], expert_down[index])
        weights = jnp.where(valid, flat_weights[order], jnp.zeros_like(flat_weights[order]))
        return (carry.at[token_ids].add(weights[:, None] * result), None)
    routed, _ = lax.scan(one_expert, jnp.zeros((batch_size, width), jnp.float32), jnp.arange(expert_gate.shape[0], dtype=jnp.int32))
    mixed = (middle + branch[:, None] * dense + routed).astype(jnp.bfloat16)
    return (mixed, new_state)
```

```python
import jax
import jax.numpy as jnp
from jax import lax
from jax.sharding import PartitionSpec as P

EPSILON = 1e-06
TAU_DECAY = 16.0


def rms_factor(values):
    return lax.rsqrt(jnp.mean(values * values, axis=-1, keepdims=True) + EPSILON)


def rounded(values):
    return lax.optimization_barrier(values.astype(jnp.bfloat16)).astype(jnp.float32)


def matmul(left, right):
    return jnp.dot(left, right, preferred_element_type=jnp.float32)


def swap(values, axis, distance):
    size = lax.axis_size(axis)
    return lax.ppermute(values, axis, [(i, i ^ distance) for i in range(size)])


def lanes_of(values, owner, size, dim):
    return lax.dynamic_slice_in_dim(values, owner * size, size, dim)


def gather_tp(piece):
    pieces = [piece]
    step = lax.axis_size("tp") // 2
    held = {0: piece}
    while step:
        for key, value in list(held.items()):
            held[key ^ step] = swap(value, "tp", step)
        step //= 2
    return [held[k] for k in range(lax.axis_size("tp"))]


def body(
    hidden_in,
    carried_state,
    input_gain,
    query_weight,
    key_weight,
    value_weight,
    outgate_weight,
    decay_weight,
    decay_shift,
    head_gain,
    output_weight,
    channel_gain,
    branch_gate,
    routes,
    route_weights,
    expert_gate,
    expert_up,
    expert_down,
    dense_gate,
    dense_up,
    dense_down,
):
    tokens_here, width = hidden_in.shape
    heads_here, key_dim, value_dim = carried_state.shape[1:]
    quarter = width // lax.axis_size("tp")
    tp_size = lax.axis_size("tp")
    ep_size = lax.axis_size("ep")
    tp_here = lax.axis_index("tp")
    ep_here = lax.axis_index("ep")
    owners = [tp_here ^ k for k in range(tp_size)]
    topk = routes.shape[1]
    capacity = tokens_here * topk // ep_size + 2
    unit_width = dense_gate.shape[1] // tp_size
    dense_in = []
    for k in range(tp_size):
        part = jnp.concatenate(
            [
                lanes_of(dense_gate, owners[k], unit_width, 1),
                lanes_of(dense_up, owners[k], unit_width, 1),
            ],
            axis=1,
        )
        dense_in.append(swap(part, "tp", k) if k else part)
    plan_own = jnp.concatenate([routes.astype(jnp.float32).T, route_weights.T], axis=0)
    plan = jnp.stack([swap(plan_own, "ep", k) if k else plan_own for k in range(ep_size)])
    hit = plan[:, :topk, :] == ep_here.astype(jnp.float32)
    token_weight = jnp.sum(jnp.where(hit, plan[:, topk:, :], 0.0), axis=1)
    hit_any = jnp.any(hit, axis=1)
    before = (
        lax.broadcasted_iota(jnp.int32, (tokens_here, tokens_here), 0)
        < lax.broadcasted_iota(jnp.int32, (tokens_here, tokens_here), 1)
    ).astype(jnp.bfloat16)
    slot = matmul(hit_any.astype(jnp.bfloat16), before).astype(jnp.int32)
    block = lax.broadcasted_iota(jnp.int32, (ep_size, tokens_here), 0)
    target = jnp.where(hit_any, block * capacity + slot, -1).reshape(1, ep_size * tokens_here)
    selector = (
        lax.broadcasted_iota(jnp.int32, (ep_size * capacity, ep_size * tokens_here), 0) == target
    ).astype(jnp.bfloat16)
    token_weight = token_weight.reshape(ep_size * tokens_here, 1)
    inputs = hidden_in.astype(jnp.float32)
    normed = (inputs * rms_factor(inputs) * input_gain.astype(jnp.float32)).astype(jnp.bfloat16)
    query = matmul(normed, query_weight).astype(jnp.bfloat16)
    key_rows = matmul(normed, key_weight).astype(jnp.bfloat16)
    value_rows = matmul(normed, value_weight).astype(jnp.bfloat16)
    outgate = matmul(normed, outgate_weight).astype(jnp.bfloat16)
    decay = jnp.exp(jax.nn.log_sigmoid(matmul(normed, decay_weight)) / TAU_DECAY + decay_shift)
    decay = decay.reshape(tokens_here, heads_here, key_dim)
    query_scaled = query.astype(jnp.float32).reshape(
        tokens_here, heads_here, key_dim
    ) * key_dim ** (-0.5)
    key_vals = key_rows.astype(jnp.float32).reshape(tokens_here, heads_here, key_dim)
    value_vals = value_rows.astype(jnp.float32).reshape(tokens_here, heads_here, value_dim)
    new_state = decay[..., None] * carried_state + key_vals[..., None] * value_vals[:, :, None, :]
    readout = jnp.einsum("bhk,bhkv->bhv", query_scaled, new_state, precision=lax.Precision.HIGHEST)
    gate_vals = jax.nn.silu(outgate.astype(jnp.float32).reshape(tokens_here, heads_here, value_dim))
    gated = (readout * rms_factor(readout) * head_gain.astype(jnp.float32) * gate_vals).astype(
        jnp.bfloat16
    )
    partial_out = rounded(matmul(gated.reshape(tokens_here, heads_here * value_dim), output_weight))
    partial_out = partial_out.astype(jnp.bfloat16)
    inputs_own = lanes_of(hidden_in, tp_here, quarter, 1).astype(jnp.float32)
    attended_own = lanes_of(partial_out, tp_here, quarter, 1).astype(jnp.float32)
    for k in range(1, tp_size):
        attended_own += swap(lanes_of(partial_out, owners[k], quarter, 1), "tp", k).astype(
            jnp.float32
        )
    middle_own = (inputs_own + attended_own).astype(jnp.bfloat16)
    blocks = [swap(middle_own, "ep", k) if k else middle_own for k in range(ep_size)]
    per_group = max(1, ep_size // 4)
    groups = [
        gather_tp(jnp.concatenate(blocks[start : start + per_group], axis=0))
        for start in range(0, ep_size, per_group)
    ]
    middle = [
        jnp.concatenate([group[k] for group in groups], axis=0).astype(jnp.float32)
        for k in range(tp_size)
    ]
    gains = [lanes_of(channel_gain, owners[k], quarter, 0).astype(jnp.float32) for k in range(tp_size)]
    gates = [lanes_of(branch_gate, owners[k], quarter, 0).astype(jnp.float32) for k in range(tp_size)]
    total_squares = sum(jnp.sum(m * m, axis=-1, keepdims=True) for m in middle)
    gate_inner = sum(
        jnp.sum(m * (g * b), axis=-1, keepdims=True) for m, g, b in zip(middle, gains, gates)
    )
    factor = lax.rsqrt(total_squares / width + EPSILON)
    branch = jax.nn.sigmoid(gate_inner * factor)
    ffn = [(m * factor * g).astype(jnp.bfloat16) for m, g in zip(middle, gains)]
    rows = jnp.zeros((ep_size * capacity, width), jnp.bfloat16)
    for k in range(tp_size):
        rows = lax.dynamic_update_slice_in_dim(
            rows, matmul(selector, ffn[k]).astype(jnp.bfloat16), owners[k] * quarter, 1
        )
    paired = sum(matmul(f, w) for f, w in zip(ffn, dense_in))
    dense_hidden = (jax.nn.silu(paired[:, :unit_width]) * paired[:, unit_width:]).astype(
        jnp.bfloat16
    )
    hidden_parts = [swap(dense_hidden, "tp", k) if k else dense_hidden for k in range(tp_size)]
    gate_part = matmul(rows, expert_gate[0])
    up_part = matmul(rows, expert_up[0])
    hidden = (jax.nn.silu(gate_part) * up_part).astype(jnp.bfloat16)
    block_out = matmul(hidden, expert_down[0]).astype(jnp.bfloat16)
    summed = lanes_of(block_out, tp_here, quarter, 1).astype(jnp.float32)
    for k in range(1, tp_size):
        summed += swap(lanes_of(block_out, owners[k], quarter, 1), "tp", k).astype(jnp.float32)
    dense_part = sum(
        matmul(h, lanes_of(dense_down, owners[k], unit_width, 0))
        for k, h in enumerate(hidden_parts)
    )
    spread = lax.dot_general(
        selector,
        summed.astype(jnp.bfloat16),
        (((0,), (0,)), ((), ())),
        preferred_element_type=jnp.float32,
    )
    joined = (branch * dense_part + token_weight * spread).astype(jnp.bfloat16)
    mixed = middle_own.astype(jnp.float32) + joined[:tokens_here].astype(jnp.float32)
    for k in range(1, ep_size):
        mixed += swap(
            joined[k * tokens_here : (k + 1) * tokens_here], "ep", k
        ).astype(jnp.float32)
    return (mixed.astype(jnp.bfloat16), new_state)


def solution(mesh):
    in_specs = (
        P("ep", None),
        P("ep", "tp", None, None),
        P(),
        P(None, "tp"),
        P(None, "tp"),
        P(None, "tp"),
        P(None, "tp"),
        P(None, "tp"),
        P("ep", "tp"),
        P("tp", None),
        P("tp", None),
        P(),
        P(),
        P("ep", None),
        P("ep", None),
        P("ep", None, "tp"),
        P("ep", None, "tp"),
        P("ep", "tp", None),
        P("tp", "ep"),
        P("tp", "ep"),
        P("ep", "tp"),
    )
    out_specs = (P("ep", "tp"), P("ep", "tp", None, None))
    return jax.shard_map(body, mesh=mesh, in_specs=in_specs, out_specs=out_specs, check_vma=False)
```

```python
import jax
import jax.numpy as jnp
from jax import lax
from jax.sharding import PartitionSpec as P

EPSILON = 1e-06
TAU_DECAY = 16.0
LANES = 128
GROUPS = 2


def rms_factor(values):
    return lax.rsqrt(jnp.mean(values * values, axis=-1, keepdims=True) + EPSILON)


def rounded(values):
    return lax.optimization_barrier(values.astype(jnp.bfloat16)).astype(jnp.float32)


def matmul(left, right):
    return jnp.dot(left, right, preferred_element_type=jnp.float32)


def swap(values, axis, distance):
    size = lax.axis_size(axis)
    return lax.ppermute(values, axis, [(i, i ^ distance) for i in range(size)])


def lanes_of(values, owner, size, dim):
    return lax.dynamic_slice_in_dim(values, owner * size, size, dim)


def gather_tp(piece):
    pieces = [piece]
    step = lax.axis_size("tp") // 2
    held = {0: piece}
    while step:
        for key, value in list(held.items()):
            held[key ^ step] = swap(value, "tp", step)
        step //= 2
    return [held[k] for k in range(lax.axis_size("tp"))]


def body(
    hidden_in,
    carried_state,
    input_gain,
    query_weight,
    key_weight,
    value_weight,
    outgate_weight,
    decay_weight,
    decay_shift,
    head_gain,
    output_weight,
    channel_gain,
    branch_gate,
    routes,
    route_weights,
    expert_gate,
    expert_up,
    expert_down,
    dense_gate,
    dense_up,
    dense_down,
):
    tokens_here, width = hidden_in.shape
    heads_here, key_dim, value_dim = carried_state.shape[1:]
    quarter = width // lax.axis_size("tp")
    tp_size = lax.axis_size("tp")
    ep_size = lax.axis_size("ep")
    tp_here = lax.axis_index("tp")
    ep_here = lax.axis_index("ep")
    owners = [tp_here ^ k for k in range(tp_size)]
    topk = routes.shape[1]
    capacity = tokens_here * topk // ep_size + 2
    unit_width = dense_gate.shape[1] // tp_size
    dense_in = []
    for k in range(tp_size):
        part = jnp.concatenate(
            [
                lanes_of(dense_gate, owners[k], unit_width, 1),
                lanes_of(dense_up, owners[k], unit_width, 1),
            ],
            axis=1,
        )
        dense_in.append(swap(part, "tp", k) if k else part)
    total = ep_size * tokens_here
    pieces = []
    left = route_weights
    for _ in range(3):
        top = lax.reduce_precision(left, 8, 7)
        pieces.append(top.astype(jnp.bfloat16))
        left = left - top
    plan_own = jnp.concatenate([routes.astype(jnp.bfloat16)] + pieces, axis=1)
    plan_own = jnp.pad(plan_own, ((0, 0), (0, LANES - plan_own.shape[1])))
    later = lax.broadcasted_iota(jnp.int32, (total, total), 0)
    sooner = lax.broadcasted_iota(jnp.int32, (total, total), 1)
    before = ((sooner < later) & (sooner // tokens_here == later // tokens_here)).astype(
        jnp.bfloat16
    )
    inputs = hidden_in.astype(jnp.float32)
    normed = (inputs * rms_factor(inputs) * input_gain.astype(jnp.float32)).astype(jnp.bfloat16)
    query = matmul(normed, query_weight).astype(jnp.bfloat16)
    key_rows = matmul(normed, key_weight).astype(jnp.bfloat16)
    value_rows = matmul(normed, value_weight).astype(jnp.bfloat16)
    outgate = matmul(normed, outgate_weight).astype(jnp.bfloat16)
    decay = jnp.exp(jax.nn.log_sigmoid(matmul(normed, decay_weight)) / TAU_DECAY + decay_shift)
    decay = decay.reshape(tokens_here, heads_here, key_dim)
    query_scaled = query.astype(jnp.float32).reshape(
        tokens_here, heads_here, key_dim
    ) * key_dim ** (-0.5)
    key_vals = key_rows.astype(jnp.float32).reshape(tokens_here, heads_here, key_dim)
    value_vals = value_rows.astype(jnp.float32).reshape(tokens_here, heads_here, value_dim)
    new_state = decay[..., None] * carried_state + key_vals[..., None] * value_vals[:, :, None, :]
    readout = jnp.einsum("bhk,bhkv->bhv", query_scaled, new_state, precision=lax.Precision.HIGHEST)
    gate_vals = jax.nn.silu(outgate.astype(jnp.float32).reshape(tokens_here, heads_here, value_dim))
    gated = (readout * rms_factor(readout) * head_gain.astype(jnp.float32) * gate_vals).astype(
        jnp.bfloat16
    )
    partial_out = rounded(matmul(gated.reshape(tokens_here, heads_here * value_dim), output_weight))
    partial_out = partial_out.astype(jnp.bfloat16)
    inputs_own = lanes_of(hidden_in, tp_here, quarter, 1).astype(jnp.float32)
    attended_own = lanes_of(partial_out, tp_here, quarter, 1).astype(jnp.float32)
    for k in range(1, tp_size):
        attended_own += swap(lanes_of(partial_out, owners[k], quarter, 1), "tp", k).astype(
            jnp.float32
        )
    middle_own = (inputs_own + attended_own).astype(jnp.bfloat16)
    payload = jnp.concatenate([middle_own, plan_own], axis=1)
    blocks = [swap(payload, "ep", k) if k else payload for k in range(ep_size)]
    per_group = max(1, ep_size // GROUPS)
    joint = [
        jnp.concatenate(blocks[start : start + per_group], axis=0)
        for start in range(0, ep_size, per_group)
    ]
    groups = [gather_tp(rows[:, :quarter]) for rows in joint]
    plan = jnp.concatenate([rows[:, quarter:] for rows in joint], axis=0).astype(jnp.float32)
    hit = plan[:, :topk] == ep_here.astype(jnp.float32)
    weight = sum(plan[:, topk * k : topk * (k + 1)] for k in (3, 2, 1))
    token_weight = jnp.sum(jnp.where(hit, weight, 0.0), axis=1, keepdims=True)
    hit_any = jnp.any(hit, axis=1, keepdims=True)
    slot = matmul(
        before, jnp.broadcast_to(hit_any, (total, LANES)).astype(jnp.bfloat16)
    )[:, :1].astype(jnp.int32)
    block = lax.broadcasted_iota(jnp.int32, (total, 1), 0) // tokens_here
    target = jnp.where(hit_any, block * capacity + slot, -1)
    selector = (
        lax.broadcasted_iota(jnp.int32, (total, ep_size * capacity), 1) == target
    ).astype(jnp.bfloat16)
    middle = [
        jnp.concatenate([group[k] for group in groups], axis=0).astype(jnp.float32)
        for k in range(tp_size)
    ]
    gains = [lanes_of(channel_gain, owners[k], quarter, 0).astype(jnp.float32) for k in range(tp_size)]
    gates = [lanes_of(branch_gate, owners[k], quarter, 0).astype(jnp.float32) for k in range(tp_size)]
    total_squares = sum(jnp.sum(m * m, axis=-1, keepdims=True) for m in middle)
    gate_inner = sum(
        jnp.sum(m * (g * b), axis=-1, keepdims=True) for m, g, b in zip(middle, gains, gates)
    )
    factor = lax.rsqrt(total_squares / width + EPSILON)
    branch = jax.nn.sigmoid(gate_inner * factor)
    ffn = [(m * factor * g).astype(jnp.bfloat16) for m, g in zip(middle, gains)]
    rows = jnp.zeros((ep_size * capacity, width), jnp.bfloat16)
    for k in range(tp_size):
        picked = lax.dot_general(
            selector, ffn[k], (((0,), (0,)), ((), ())), preferred_element_type=jnp.float32
        )
        rows = lax.dynamic_update_slice_in_dim(
            rows, picked.astype(jnp.bfloat16), owners[k] * quarter, 1
        )
    paired = sum(matmul(f, w) for f, w in zip(ffn, dense_in))
    dense_hidden = (jax.nn.silu(paired[:, :unit_width]) * paired[:, unit_width:]).astype(
        jnp.bfloat16
    )
    hidden_parts = [swap(dense_hidden, "tp", k) if k else dense_hidden for k in range(tp_size)]
    gate_part = matmul(rows, expert_gate[0])
    up_part = matmul(rows, expert_up[0])
    hidden = (jax.nn.silu(gate_part) * up_part).astype(jnp.bfloat16)
    block_out = matmul(hidden, expert_down[0]).astype(jnp.bfloat16)
    summed = lanes_of(block_out, tp_here, quarter, 1).astype(jnp.float32)
    for k in range(1, tp_size):
        summed += swap(lanes_of(block_out, owners[k], quarter, 1), "tp", k).astype(jnp.float32)
    dense_part = sum(
        matmul(h, lanes_of(dense_down, owners[k], unit_width, 0))
        for k, h in enumerate(hidden_parts)
    )
    spread = matmul(selector, summed.astype(jnp.bfloat16))
    joined = (branch * dense_part + token_weight * spread).astype(jnp.bfloat16)
    mixed = middle_own.astype(jnp.float32) + joined[:tokens_here].astype(jnp.float32)
    for k in range(1, ep_size):
        mixed += swap(
            joined[k * tokens_here : (k + 1) * tokens_here], "ep", k
        ).astype(jnp.float32)
    return (mixed.astype(jnp.bfloat16), new_state)


def solution(mesh):
    in_specs = (
        P("ep", None),
        P("ep", "tp", None, None),
        P(),
        P(None, "tp"),
        P(None, "tp"),
        P(None, "tp"),
        P(None, "tp"),
        P(None, "tp"),
        P("ep", "tp"),
        P("tp", None),
        P("tp", None),
        P(),
        P(),
        P("ep", None),
        P("ep", None),
        P("ep", None, "tp"),
        P("ep", None, "tp"),
        P("ep", "tp", None),
        P("tp", "ep"),
        P("tp", "ep"),
        P("ep", "tp"),
    )
    out_specs = (P("ep", "tp"), P("ep", "tp", None, None))
    return jax.shard_map(body, mesh=mesh, in_specs=in_specs, out_specs=out_specs, check_vma=False)
```
